32 devices in a mesh: row: 8 (over z, core), col: 4 (over y, x).
Axes of the slice: x: 2, y: 2, z: 4, core: 2. Of those that a mesh axis runs over, the one named last changes fastest.
Arguments:
- tokens: bfloat16 [4096, 4096], P('row', 'col'), may hold values from -6 to 6
- norm_gain: float32 [4096], replicated, may hold values from 0.1 to 1.9
- out_weight: bfloat16 [4096, 4096], P(None, 'col'), may hold values from -0.09375 to 0.09375
Outputs:
- mixed: bfloat16 [4096, 4096], P('row', 'col')
The draws below stay inside these ranges and needn't reach their ends.
All inputs are finite; a program needn't handle non-finite values.
Results may differ from the reference program's by a relative error of at most 0.015.
Values may be sent and summed in bfloat16 or wider, within the bound.
A program may use at most 64 MiB of HBM per device.

```python
import jax
import jax.numpy as jnp
from jax import lax

D = 4096
GROUPS = 4
CG = 1024
SEQ = 4096


def block_levels(key, shape, shards, low, high):
    def one(position, shards_of):
        heights = jax.random.uniform(jax.random.fold_in(jax.random.fold_in(key, 6), position), (shards_of,), jnp.float32, low / len(shards), high / len(shards))
        return jnp.repeat(jnp.exp(heights), shape[position] // shards_of).reshape((-1,) + (1,) * (len(shape) - position - 1))

    level = one(*shards[0])
    for cut in shards[1:]:
        level = level * one(*cut)
    return level


def scatter_about(own_key, dims, width, reach, cuts=(), held_as=jnp.bfloat16):
    result = jax.random.normal(own_key, dims, jnp.float32) * width
    if len(cuts) > 0:
        result = block_levels(own_key, dims, cuts, -0.22, 0.18) * result
    return jnp.clip(result, min=-reach, max=reach).astype(held_as)


def setup_inputs(seed: int = 0) -> dict:
    key_of = jax.random.split(jax.random.key(seed), 4)
    return {
        "tokens": scatter_about(key_of[0], (SEQ, D), 1.0, 6.0, ((0, 8), (1, 4))),
        "norm_gain": jnp.clip(1.0 + 0.18 * jax.random.normal(key_of[1], (D,), jnp.float32), 0.1, 1.9),
        "out_weight": scatter_about(key_of[2], (D, D), D ** -0.5, 0.09375, ((1, 4),)),
    }


def reference(tokens, norm_gain, out_weight):
    values = tokens.astype(jnp.float32)
    inv_rms = lax.rsqrt(lax.optimization_barrier(jnp.mean(values * values, axis=-1, keepdims=True)) + 1e-06)
    normed = lax.optimization_barrier((values * inv_rms * norm_gain).astype(jnp.bfloat16))
    grouped = normed.astype(jnp.float32).reshape(SEQ, GROUPS, CG)
    spectrum = jnp.fft.fftn(grouped, axes=(0, 2), norm='ortho').real
    mixed_in = spectrum.reshape(SEQ, D).astype(jnp.bfloat16)
    return jnp.dot(mixed_in, out_weight, preferred_element_type=jnp.float32).astype(jnp.bfloat16)
```

```python
import functools
import math

import numpy as np

import jax
import jax.numpy as jnp
from jax import lax
from jax.experimental import pallas as pl
from jax.experimental.pallas import tpu as pltpu
from jax.sharding import PartitionSpec as P

GROUPS = 4


EPSILON = 1e-06
PRECISE = lax.Precision.HIGHEST


def phases(left_idx, right_idx, period):
    product = left_idx[:, None] * right_idx[None, :] % period
    angles = product.astype(jnp.float32) * (2.0 * math.pi / period)
    return (jnp.cos(angles), jnp.sin(angles))


def split_table(table):
    table_high = table.astype(jnp.bfloat16)
    remainder = table - table_high.astype(jnp.float32)
    table_middle = remainder.astype(jnp.bfloat16)
    table_low = (remainder - table_middle.astype(jnp.float32)).astype(jnp.bfloat16)
    return (table_high, table_middle, table_low)


def host_tables(group_len, row_count, block_len):
    seq_len = block_len * row_count
    half = group_len // 2 // row_count
    slot = np.arange(group_len)
    freq = (slot // (2 * half)) * half + slot % half
    odd = slot // half % 2 == 1
    nyquist = odd & (freq == 0)
    sine = odd & ~nyquist
    freq = np.where(nyquist, group_len // 2, freq)
    chan = np.arange(group_len)
    angle = 2 * np.pi * (chan[:, None] * freq[None, :] % group_len) / group_len
    chan_table = np.where(sine[None, :], np.sin(angle), np.cos(angle)) / np.sqrt(group_len)
    low = np.arange(block_len)
    angle = 2 * np.pi * (low[:, None] * low[None, :] % block_len) / block_len
    low_table = np.concatenate([np.cos(angle), np.sin(angle)], 1) / np.sqrt(seq_len)
    high = np.arange(row_count)
    angle = 2 * np.pi * (high[:, None] * low[None, :] % seq_len) / seq_len
    return chan_table, low_table, np.cos(angle), np.sin(angle)


def slot_facts(slot, group_len, row_count):
    half = group_len // 2 // row_count
    freq = (slot // (2 * half)) * half + slot % half
    odd = slot // half % 2 == 1
    nyquist = odd & (freq == 0)
    return jnp.where(nyquist, group_len // 2, freq), odd & ~nyquist


def folding(group_len, row_count):
    freq, sine = slot_facts(jnp.arange(group_len, dtype=jnp.int32), group_len, row_count)
    chan = jnp.arange(group_len, dtype=jnp.int32)[None, :]
    direct = chan == freq[:, None]
    mirror = chan == ((group_len - freq) % group_len)[:, None]
    signed = jnp.where(sine[:, None], -1.0, 1.0)
    return jnp.where(direct, signed, jnp.where(mirror, 1.0, 0.0)).astype(jnp.bfloat16)


def on_device_folded(tokens, norm_gain, out_weight):
    row_count = lax.axis_size("row")
    col_count = lax.axis_size("col")
    block_len, group_len = tokens.shape
    full_width = group_len * col_count
    slab = group_len // row_count
    out_width = out_weight.shape[1]
    chan_table, low_table, twist_cos, twist_sin = host_tables(group_len, row_count, block_len)
    chan_table = jnp.asarray(chan_table, jnp.bfloat16)
    low_table = jnp.asarray(low_table, jnp.bfloat16)
    twist_cos = jnp.asarray(twist_cos, jnp.float32)[:, :, None]
    twist_sin = jnp.asarray(twist_sin, jnp.float32)[:, :, None]
    values = tokens.astype(jnp.float32)
    total = lax.psum(jnp.sum(values * values, axis=-1), "col")
    inv_rms = lax.rsqrt(total / full_width + EPSILON)[:, None]
    gain = lax.dynamic_slice_in_dim(norm_gain, lax.axis_index("col") * group_len, group_len)
    normed = (values * inv_rms * gain).astype(jnp.bfloat16)
    chans = jnp.dot(normed, chan_table, preferred_element_type=jnp.float32).astype(jnp.bfloat16)
    moved = lax.all_to_all(chans, "row", split_axis=1, concat_axis=0, tiled=True)
    blocks = moved.reshape(row_count, block_len, slab).astype(jnp.float32)
    _, sine = slot_facts(
        lax.axis_index("row") * slab + jnp.arange(slab, dtype=jnp.int32), group_len, row_count
    )
    tops, bottoms = [], []
    for q in range(row_count):
        real, imag = 0.0, 0.0
        for a in range(row_count):
            angle = 2 * math.pi * (a * q % row_count) / row_count
            real = real + blocks[a] * round(math.cos(angle), 12)
            imag = imag - blocks[a] * round(math.sin(angle), 12)
        turned_real = real * twist_cos[q] + imag * twist_sin[q]
        turned_imag = imag * twist_cos[q] - real * twist_sin[q]
        tops.append(jnp.where(sine, -turned_imag, turned_real).astype(jnp.bfloat16))
        bottoms.append(jnp.where(sine, turned_real, turned_imag).astype(jnp.bfloat16))
    stacked = jnp.concatenate([jnp.concatenate(tops, 1), jnp.concatenate(bottoms, 1)], 0)
    lows = jnp.dot(low_table, stacked, preferred_element_type=jnp.float32).astype(jnp.bfloat16)
    back = lax.all_to_all(
        lows.reshape(row_count, block_len // row_count, row_count * slab),
        "row", split_axis=0, concat_axis=0, tiled=True,
    )
    gathered = lax.all_gather(back, "col", axis=0, tiled=False)
    fold = folding(group_len, row_count)
    folded = jnp.einsum(
        "sm,gme->gse", fold, out_weight.reshape(col_count, group_len, out_width),
        preferred_element_type=jnp.float32,
    ).astype(jnp.bfloat16)
    mapped = jnp.einsum(
        "gspql,gsle->pqe",
        gathered.reshape(col_count, row_count, block_len // row_count, row_count, slab),
        folded.reshape(col_count, row_count, slab, out_width),
        preferred_element_type=jnp.float32,
    )
    return mapped.astype(jnp.bfloat16).reshape(block_len, out_width)


MESH = pl.DeviceIdType.MESH
F32 = jnp.float32
BF16 = jnp.bfloat16
WIDTHS = (16, 32, 32, 16, 16, 16)
NEAR_FIRST = (True, True, True, True, True, True)
FOLDS = (0, 6, 11, 16)
PLAN = (
    "A0", "A1", "F0", "I", "A2", "D0", "D1", "Gn0", "Gf0", "Gn1", "A3", "D2", "F1", "Xn0", "Xn1", "Gf1",
    "Xf0", "Gn2", "Xf1", "A4", "D3", "Gf2", "Xn2", "F2", "A5", "D4", "Gn3", "Mf0", "Gf3", "Mf1", "Xf2",
    "Mn0", "Xn3", "D5", "Xf3", "Gn4", "Mn1", "Gf4", "Mn3", "Gn5", "Mf3", "Xn4", "Xf4", "Mf2", "Gf5", "Xn5",
    "Mn2", "Mn4", "Xf5", "Mf4", "Mn5", "Mf5",
)


def fused_tables(group_len, row_count, block_len):
    seq_len = block_len * row_count
    freqs, sines = [], []
    offset = 0
    for width in WIDTHS:
        half = width // 2
        slot = np.arange(row_count * width)
        freqs.append(row_count // 2 * offset + slot // width * half + slot % half)
        sines.append(slot % width >= half)
        offset += width
    freq, odd = np.concatenate(freqs), np.concatenate(sines)
    nyquist = odd & (freq == 0)
    sine = odd & ~nyquist
    freq = np.where(nyquist, group_len // 2, freq)
    chan = np.arange(group_len)
    angle = 2 * np.pi * (freq[:, None] * chan[None, :] % group_len) / group_len
    chan_table = np.where(sine[:, None], np.sin(angle), np.cos(angle)) / np.sqrt(group_len)
    low = np.arange(block_len)
    angle = 2 * np.pi * (low[:, None] * low[None, :] % block_len) / block_len
    low_table = np.concatenate([np.cos(angle), np.sin(angle)], 0) / np.sqrt(seq_len)
    high = np.arange(row_count)
    angle = 2 * np.pi * (high[:, None] * low[None, :] % seq_len) / seq_len
    return chan_table, low_table, np.concatenate([np.cos(angle), np.sin(angle)], 0)


def fused_kernel(
    dims, x_hbm, gain_ref, table_hbm, low_hbm, twist_ref, w_hbm, out_ref,
    x_ref, scaled, table_ref, low_ref, w_ref, fold_ref, folded, send1, recv1, sums, invs, stacked, send2,
    held, lhs, acc,
    l_sem, stay_sem, send_sem, s_recv, i_recv, a_recv, b_recv, g_recv,
):
    row_count, col_count = dims
    block_len, group_len = x_ref.shape
    full_width = group_len * col_count
    out_width = out_ref.shape[2]
    part = block_len // row_count
    slab = group_len // row_count
    chunks = len(WIDTHS)
    offsets = [sum(WIDTHS[:i]) for i in range(chunks)]
    quads = row_count // 2
    r = lax.axis_index("row")
    c = lax.axis_index("col")
    core, inner, side = r % 2, r // 2 % 2, r // 4

    def peer_of(d):
        k = 1 - core if d % 2 else core
        t = 1 - inner if d // 2 % 2 else inner
        s = 1 - side if d // 4 else side
        return 4 * s + 2 * t + k

    x_next = 2 * (c // 2) + 1 - c % 2
    y_next = 2 * (1 - c // 2) + c % 2
    diagonal = 2 * (1 - c // 2) + 1 - c % 2
    col_peers = (x_next, y_next, diagonal)
    near, far = tuple(range(1, quads)), tuple(range(quads, row_count))

    def rows_of(start, size, unit):
        return pl.ds(pl.multiple_of(start, unit), size)

    x_copy = pltpu.make_async_copy(x_hbm, x_ref, l_sem.at[0])
    early = row_count * WIDTHS[0]
    table_copy = pltpu.make_async_copy(table_hbm.at[:early], table_ref.at[:early], l_sem.at[1])
    table_rest = pltpu.make_async_copy(table_hbm.at[early:], table_ref.at[early:], l_sem.at[4])
    low_copy = pltpu.make_async_copy(low_hbm, low_ref, l_sem.at[2])
    w_copy = pltpu.make_async_copy(w_hbm, w_ref, l_sem.at[3])
    x_copy.start()
    table_copy.start()

    barrier = pltpu.get_barrier_semaphore()
    for d in range(1, row_count):
        pl.semaphore_signal(barrier, inc=1, device_id=(peer_of(d), c), device_id_type=MESH)
    for peer in col_peers:
        pl.semaphore_signal(barrier, inc=1, device_id=(r, peer), device_id_type=MESH)

    lanes = (((1,), (1,)), ((), ()))
    x_copy.wait()
    for copy in (table_rest, low_copy, w_copy):
        copy.start()
    values = x_ref[...].astype(F32)
    gain = gain_ref[:, pl.ds(pl.multiple_of(c * group_len, group_len), group_len)]
    scaled[...] = (values * gain).astype(BF16)

    def remote(source, target_ref, phase, recv_sem, device):
        pltpu.make_async_remote_copy(
            src_ref=source, dst_ref=target_ref, send_sem=send_sem.at[phase], recv_sem=recv_sem,
            device_id=device, device_id_type=MESH,
        ).start()

    def sent(ref, phase):
        pltpu.make_async_remote_copy(
            src_ref=ref, dst_ref=ref, send_sem=send_sem.at[phase], recv_sem=l_sem.at[0],
            device_id=(peer_of(1), c), device_id_type=MESH,
        ).wait_send()

    def arrived(ref, semaphore):
        pltpu.make_async_remote_copy(
            src_ref=ref, dst_ref=ref, send_sem=l_sem.at[0], recv_sem=semaphore,
            device_id=(peer_of(1), c), device_id_type=MESH,
        ).wait_recv()

    first_stays, second_stays = {}, {}

    def features(i):
        width, offset = WIDTHS[i], offsets[i]
        rows = pl.ds(row_count * offset, row_count * width)
        send1[rows, :] = lax.dot_general(
            table_ref[rows, :], scaled[...], lanes, preferred_element_type=F32
        ).astype(BF16)

    def first_exchange(i):
        width, offset = WIDTHS[i], offsets[i]
        if i == 0:
            square_sums()
            table_copy.wait()
        if i == 1:
            table_rest.wait()
        features(i)
        if i == 0:
            pl.semaphore_wait(barrier, row_count + col_count - 2)
            for peer in col_peers:
                remote(sums.at[c], sums.at[c], 0, s_recv.at[0], (r, peer))
        target = recv1.at[r, pl.ds(offset, width), :]
        for d in far + near[::-1]:
            peer = peer_of(d)
            source = send1.at[rows_of(row_count * offset + peer * width, width, 16), :]
            remote(source, target, 2, a_recv.at[i], (peer, c))
        source = send1.at[rows_of(row_count * offset + r * width, width, 16), :]
        first_stays[i] = pltpu.make_async_copy(source, target, stay_sem.at[0, i])
        first_stays[i].start()

    def square_sums():
        squares = x_ref[...].astype(F32)
        squares = squares * squares
        top = squares.astype(BF16)
        rest = (squares - top.astype(F32)).astype(BF16)
        ones = jnp.ones((16, group_len), BF16)
        own = lax.dot_general(ones, top, lanes, preferred_element_type=F32)
        own = own + lax.dot_general(ones, rest, lanes, preferred_element_type=F32)
        sums[c] = own[:1]

    def inverses():
        arrived(sums.at[: col_count - 1], s_recv.at[0])
        total = sums[0]
        for k in range(1, col_count):
            total = total + sums[k]
        invs[r] = lax.rsqrt(total / full_width + EPSILON)
        for d in far + near[::-1]:
            remote(invs.at[r], invs.at[r], 1, i_recv.at[0], (peer_of(d), c))

    def butterfly(i):
        width, offset = WIDTHS[i], offsets[i]
        half = width // 2
        middle = row_count // 2

        def step(j, carry):
            spot = rows_of(j * 128, 128, 128)
            below = rows_of(block_len + j * 128, 128, 128)
            for base in range(0, width, 16):
                rows = pl.ds(offset + base, 16)
                blocks = [
                    recv1[a, rows, spot].astype(F32) * invs[a, :, spot] for a in range(row_count)
                ]
                even = [blocks[a] + blocks[row_count - a] for a in range(1, middle)]
                odd = [blocks[a] - blocks[row_count - a] for a in range(1, middle)]
                ends = (blocks[0] + blocks[middle], blocks[0] - blocks[middle])
                row = lax.broadcasted_iota(jnp.int32, (16, 128), 0) + base
                sine = row >= half
                if offset == 0:
                    sine = (row > half) | ((row == half) & (r > 0))
                plain = base + 16 <= half
                turned = base >= half and (offset > 0 or base > half)
                for q in range(middle + 1):
                    real = ends[q % 2]
                    imag = None
                    for a in range(1, middle):
                        angle = 2 * math.pi * (a * q % row_count) / row_count
                        cosine, sinus = round(math.cos(angle), 12), round(math.sin(angle), 12)
                        if cosine:
                            real = real + (even[a - 1] if cosine == 1 else even[a - 1] * cosine)
                        if sinus:
                            term = odd[a - 1] * -sinus
                            imag = term if imag is None else imag + term
                    for k, sign in ((q, 1.0), (row_count - q, -1.0)):
                        if k == row_count or (sign < 0 and k == q):
                            continue
                        if k == 0:
                            turned_real, turned_imag = real, jnp.zeros_like(real)
                        else:
                            cosine = twist_ref[k : k + 1, spot]
                            sinus = twist_ref[row_count + k : row_count + k + 1, spot]
                            if imag is None:
                                turned_real, turned_imag = real * cosine, -(real * sinus)
                            elif sign > 0:
                                turned_real = real * cosine + imag * sinus
                                turned_imag = imag * cosine - real * sinus
                            else:
                                turned_real = real * cosine - imag * sinus
                                turned_imag = -(imag * cosine + real * sinus)
                        if plain:
                            upper, lower = turned_real, turned_imag
                        elif turned:
                            upper, lower = -turned_imag, turned_real
                        else:
                            upper = jnp.where(sine, -turned_imag, turned_real)
                            lower = jnp.where(sine, turned_real, turned_imag)
                        place = pl.ds((k % 2 * quads + k // 2) * width + base, 16)
                        stacked[place, spot] = upper.astype(BF16)
                        stacked[place, below] = lower.astype(BF16)
            return carry

        lax.fori_loop(0, block_len // 128, step, 0)

    def second_exchange(i):
        width, offset = WIDTHS[i], offsets[i]
        lane = lax.broadcasted_iota(jnp.int32, (quads * width, 128), 1)
        first_half = lane < part
        target = held.at[c, :, rows_of(row_count * offset + r * width, width, 16), :]
        for nearby in (True, False) if NEAR_FIRST[i] else (False, True):
            where = side if nearby else 1 - side
            lows = jnp.dot(
                stacked[: row_count * width, :],
                low_ref[:, rows_of(where * (block_len // 2), block_len // 2, 256)],
                preferred_element_type=F32,
            )
            for t in range(2):
                left = lows[: quads * width, t * 128 : (t + 1) * 128]
                right = lows[quads * width :, t * 128 : (t + 1) * 128]
                pair = (
                    jnp.where(first_half, left, pltpu.roll(right, part, 1)),
                    jnp.where(first_half, pltpu.roll(left, part, 1), right),
                )
                for k in range(2):
                    value = pair[k].astype(BF16).reshape(quads, width, 128)
                    send2[4 * where + 2 * t + k, :, pl.ds(offset, width), :] = value
            for d in near[::-1] if nearby else far:
                peer = peer_of(d)
                source = send2.at[peer, :, pl.ds(offset, width), :]
                remote(source, target, 3, b_recv.at[i, 0 if nearby else 1], (peer, c))
        source = send2.at[r, :, pl.ds(offset, width), :]
        second_stays[i] = pltpu.make_async_copy(source, target, stay_sem.at[1, i])
        second_stays[i].start()

    def transform(i):
        width, offset = WIDTHS[i], offsets[i]
        first_stays[i].wait()
        if i == 0:
            low_copy.wait()
            arrived(invs.at[: row_count - 1], i_recv.at[0])
        arrived(recv1.at[: row_count - 1, pl.ds(offset, width), :], a_recv.at[i])
        butterfly(i)
        second_exchange(i)

    def place_of(i, h):
        width, offset = WIDTHS[i], offsets[i]
        where = side if h == "n" else 1 - side
        return rows_of(row_count * offset + where * quads * width, quads * width, 16)

    def piece(origin, i, h, u):
        return held.at[origin, pl.ds(2 * u, 2), place_of(i, h), :]

    def spread(i, h, u, origin, target, kind):
        slot = 2 * i + (h == "f")
        part_ref = piece(origin, i, h, u)
        remote(part_ref, part_ref, 4, g_recv.at[slot, kind], (r, target))

    def came(i, h, u, origin, kind):
        arrived(piece(origin, i, h, u), g_recv.at[2 * i + (h == "f"), kind])

    def gather(i, h):
        width, offset = WIDTHS[i], offsets[i]
        if h == "n":
            arrived(held.at[c, :, pl.ds(row_count * offset, len(near) * width), :], b_recv.at[i, 0])
            second_stays[i].wait()
        else:
            arrived(held.at[c, :, pl.ds(row_count * offset, len(far) * width), :], b_recv.at[i, 1])
        spread(i, h, 0, c, x_next, 0)
        spread(i, h, 1, c, y_next, 1)
        spread(i, h, 1, c, x_next, 2)
        spread(i, h, 0, c, y_next, 2)

    def forward(i, h):
        came(i, h, 0, x_next, 0)
        spread(i, h, 0, x_next, y_next, 2)
        came(i, h, 1, y_next, 1)
        spread(i, h, 1, y_next, x_next, 2)

    wide, broad = 256, 512
    pieces = out_width // wide

    def fold_spans(i):
        width, offset = WIDTHS[i], offsets[i]
        start, count = quads * offset, quads * width
        high = min(group_len - start - count, group_len - count - 16)
        return start, count, high, 2 * count + 16 + (16 if i == 0 else 0)

    def fold_matrix(i):
        width = WIDTHS[i]
        start, count, high, depth = fold_spans(i)
        shape = (2 * count, depth)
        slot = lax.broadcasted_iota(jnp.int32, shape, 0)
        column = lax.broadcasted_iota(jnp.int32, shape, 1)
        half = width // 2
        freq = start + slot // width * half + slot % half
        odd = slot % width >= half
        nyquist = odd & (freq == 0)
        direct = (column == freq - start) & ~nyquist & (column < count)
        mirror = (column - count + high == group_len - freq) & (freq > 0)
        mirror = mirror & (column >= count) & (column < 2 * count + 16)
        middle = nyquist & (column == 2 * count + 16)
        signed = jnp.where(odd, -1.0, 1.0)
        matrix = jnp.where(direct, signed, jnp.where(mirror | middle, 1.0, 0.0)).astype(BF16)
        fold_ref[row_count * offsets[i] : row_count * (offsets[i] + width), :depth] = matrix

    def fold(m):
        if m == 0:
            for i in range(chunks):
                fold_matrix(i)
            w_copy.wait()

        def step(n, carry):
            group = n // pieces
            origin = group * group_len
            cols = rows_of(n % pieces * wide, wide, wide)
            for i in range(chunks):
                start, count, high, depth = fold_spans(i)
                base = row_count * offsets[i]
                taken = [w_ref[rows_of(origin + start, count, 16), cols]]
                taken.append(w_ref[rows_of(origin + high, count + 16, 16), cols])
                if i == 0:
                    taken.append(w_ref[rows_of(origin + group_len // 2, 16, 16), cols])
                value = jnp.dot(
                    fold_ref[base : base + 2 * count, :depth], jnp.concatenate(taken, 0),
                    preferred_element_type=F32,
                ).astype(BF16)
                for s in range(2):
                    start = base * col_count + s * col_count * count + group * count
                    folded[rows_of(start, count, 16), cols] = value[s * count : (s + 1) * count]
            return carry

        lax.fori_loop(FOLDS[m], FOLDS[m + 1], step, 0)

    done = []

    def multiply(i, h):
        width, offset = WIDTHS[i], offsets[i]
        count = quads * width
        depth = col_count * count
        arrived(held.at[:2, :, place_of(i, h), :], g_recv.at[2 * i + (h == "f"), 2])
        for g in range(col_count):
            for q in range(quads):
                lhs[q * 128 : (q + 1) * 128, g * count : (g + 1) * count] = jnp.transpose(
                    held[g, q, place_of(i, h), :]
                )
        where = side if h == "n" else 1 - side
        rows = rows_of(row_count * offset * col_count + where * depth, depth, 16)
        first, last = not done, len(done) == 2 * chunks - 1
        done.append((i, h))

        def step(n, carry):
            cols = rows_of(n * broad, broad, broad)
            value = jnp.dot(lhs[:, :depth], folded[rows, cols], preferred_element_type=F32)
            if not first:
                value = acc[:, cols] + value
            if not last:
                acc[:, cols] = value
            else:
                out_ref[:, :, cols] = value.astype(BF16).reshape(row_count, part, broad)
            return carry

        lax.fori_loop(0, out_width // broad, step, 0)

    for token in PLAN:
        i = int(token[-1]) if token[-1].isdigit() else 0
        with jax.named_scope(token):
            match token[0]:
                case "A":
                    first_exchange(i)
                case "I":
                    inverses()
                case "F":
                    fold(i)
                case "D":
                    transform(i)
                case "G":
                    gather(i, token[1])
                case "X":
                    forward(i, token[1])
                case "M":
                    multiply(i, token[1])

    sent(sums.at[: col_count - 1], 0)
    sent(invs.at[: row_count - 1], 1)
    sent(send1.at[: group_len - slab], 2)
    sent(send2.at[: row_count - 1], 3)
    sent(held.at[: col_count - 1], 4)


def on_device_fused(tokens, norm_gain, out_weight):
    row_count = lax.axis_size("row")
    col_count = lax.axis_size("col")
    block_len, group_len = tokens.shape
    out_width = out_weight.shape[1]
    slab = group_len // row_count
    part = block_len // row_count
    chunks = len(WIDTHS)
    widest = max(WIDTHS)
    chan_table, low_table, twist = fused_tables(group_len, row_count, block_len)
    vmem = pl.BlockSpec(memory_space=pltpu.VMEM)
    hbm = pl.BlockSpec(memory_space=pl.ANY)
    dma = pltpu.SemaphoreType.DMA
    mapped = pl.pallas_call(
        functools.partial(fused_kernel, (row_count, col_count)),
        out_shape=pltpu.VMEM((row_count, part, out_width), BF16),
        in_specs=[hbm, vmem, hbm, hbm, vmem, hbm],
        out_specs=vmem,
        scratch_shapes=[
            pltpu.VMEM((block_len, group_len), BF16),
            pltpu.VMEM((block_len, group_len), BF16),
            pltpu.VMEM(chan_table.shape, BF16),
            pltpu.VMEM(low_table.shape, BF16),
            pltpu.VMEM(out_weight.shape, BF16),
            pltpu.VMEM((group_len, row_count * widest + 32), BF16),
            pltpu.VMEM(out_weight.shape, BF16),
            pltpu.VMEM((group_len, block_len), BF16),
            pltpu.VMEM((row_count, slab, block_len), BF16),
            pltpu.VMEM((col_count, 1, block_len), F32),
            pltpu.VMEM((row_count, 1, block_len), F32),
            pltpu.VMEM((row_count * widest, 2 * block_len), BF16),
            pltpu.VMEM((row_count, row_count // 2, slab, 128), BF16),
            pltpu.VMEM((col_count, row_count // 2, group_len, 128), BF16),
            pltpu.VMEM((block_len, col_count * row_count // 2 * widest), BF16),
            pltpu.VMEM((block_len, out_width), F32),
            dma((5,)), dma((2, chunks)), dma((5,)), dma((1,)), dma((1,)),
            dma((chunks,)), dma((chunks, 2)), dma((2 * chunks, 3)),
        ],
        compiler_params=pltpu.CompilerParams(
            collective_id=0, has_side_effects=True, vmem_limit_bytes=60 * 1024 * 1024
        ),
    )(
        tokens, norm_gain[None, :], jnp.asarray(chan_table, BF16), jnp.asarray(low_table, BF16),
        jnp.asarray(twist, F32), out_weight,
    )
    return jnp.transpose(mapped, (1, 0, 2)).reshape(block_len, out_width)


def on_device(tokens, norm_gain, out_weight):
    row_count = lax.axis_size("row")
    col_count = lax.axis_size("col")
    block_len, local_width = tokens.shape
    full_width = local_width * col_count
    group_len = full_width // GROUPS
    share_len = block_len // col_count
    seq_len = block_len * row_count
    slab_len = full_width // row_count
    col_index = lax.axis_index("col")
    chan_idx = jnp.arange(group_len, dtype=jnp.int32)
    cosines, sines = phases(chan_idx, chan_idx, group_len)
    chan_table = jnp.concatenate([cosines, sines], axis=1) / math.sqrt(group_len)
    table_parts = split_table(chan_table)
    arranged = tokens.reshape(col_count, share_len, local_width)
    portion = lax.all_to_all(arranged, "col", split_axis=0, concat_axis=2, tiled=True)
    item_count = portion.shape[1]
    values = portion.astype(jnp.float32)
    inv_rms = lax.rsqrt(jnp.mean(values * values, axis=-1, keepdims=True) + EPSILON)
    normed = lax.optimization_barrier((values * inv_rms * norm_gain).astype(jnp.bfloat16))
    grouped = normed.reshape(item_count, GROUPS, group_len)
    result = jnp.einsum("pgm,mj->pgj", grouped, table_parts[0], preferred_element_type=jnp.float32)
    result = result + jnp.einsum(
        "pgm,mj->pgj", grouped, table_parts[1], preferred_element_type=jnp.float32
    )
    result = result + jnp.einsum(
        "pgm,mj->pgj", grouped, table_parts[2], preferred_element_type=jnp.float32
    )
    high_idx = jnp.arange(row_count, dtype=jnp.int32)
    high_cos, high_sin = phases(high_idx, high_idx, row_count)
    high_table = jnp.concatenate(
        [jnp.concatenate([high_cos, -high_sin], 1), jnp.concatenate([-high_sin, -high_cos], 1)], 0
    )
    parts = (
        lax.all_to_all(
            result[..., :group_len].reshape(1, item_count, full_width),
            "row",
            split_axis=2,
            concat_axis=0,
            tiled=True,
        ),
        lax.all_to_all(
            result[..., group_len:].reshape(1, item_count, full_width),
            "row",
            split_axis=2,
            concat_axis=0,
            tiled=True,
        ),
    )
    item_count = parts[0].shape[1]
    stacked = jnp.concatenate(parts, 0).reshape(2 * row_count, item_count * slab_len)
    result = jnp.dot(high_table, stacked, precision=PRECISE)
    real_part = result[:row_count].reshape(row_count, item_count, slab_len)
    imag_part = result[row_count:].reshape(row_count, item_count, slab_len)
    local_pos = col_index * share_len + jnp.arange(share_len, dtype=jnp.int32)
    twist_cos, twist_sin = phases(high_idx, local_pos, seq_len)
    twist_cos = twist_cos[:, :, None]
    twist_sin = twist_sin[:, :, None]
    turned_real = real_part * twist_cos + imag_part * twist_sin
    turned_imag = imag_part * twist_cos - real_part * twist_sin
    low_idx = jnp.arange(block_len, dtype=jnp.int32)
    low_cos, low_sin = phases(low_idx, low_idx, block_len)
    low_cos = low_cos / math.sqrt(seq_len)
    low_sin = low_sin / math.sqrt(seq_len)
    low_table = jnp.concatenate([low_cos, low_sin], 1)
    stacked = jnp.concatenate(
        (
            lax.all_to_all(turned_real, "col", split_axis=0, concat_axis=1, tiled=True),
            lax.all_to_all(turned_imag, "col", split_axis=0, concat_axis=1, tiled=True),
        ),
        1,
    )
    finished = (jnp.einsum("ks,asc->akc", low_table, stacked, precision=PRECISE),)[0]
    spectrum = finished.astype(jnp.bfloat16)
    returned = lax.all_to_all(spectrum, "row", split_axis=1, concat_axis=2, tiled=True)
    mapped = jnp.einsum(
        "akd,de->kae",
        lax.all_gather(returned, "col", axis=0, tiled=True),
        out_weight,
        preferred_element_type=jnp.float32,
    )
    return mapped.astype(jnp.bfloat16).reshape(block_len, local_width)


def solution(mesh):
    def body(tokens, norm_gain, out_weight):
        whole_groups = tokens.shape[1] * GROUPS == out_weight.shape[0]
        slab = tokens.shape[1] // mesh.shape["row"]
        program = on_device_folded if whole_groups else on_device
        if whole_groups and slab == 128 and mesh.shape["col"] == 4 and mesh.shape["row"] == 8:
            program = on_device_fused
        return program(tokens, norm_gain, out_weight)

    placed = (P("row", "col"), P(), P(None, "col"))
    return jax.shard_map(
        body, mesh=mesh, in_specs=placed, out_specs=P("row", "col"), check_vma=False
    )
```

```python
import functools
import math

import numpy as np

import jax
import jax.numpy as jnp
from jax import lax
from jax.experimental import pallas as pl
from jax.experimental.pallas import tpu as pltpu
from jax.sharding import PartitionSpec as P

GROUPS = 4


EPSILON = 1e-06
PRECISE = lax.Precision.HIGHEST


def phases(left_idx, right_idx, period):
    product = left_idx[:, None] * right_idx[None, :] % period
    angles = product.astype(jnp.float32) * (2.0 * math.pi / period)
    return (jnp.cos(angles), jnp.sin(angles))


def split_table(table):
    table_high = table.astype(jnp.bfloat16)
    remainder = table - table_high.astype(jnp.float32)
    table_middle = remainder.astype(jnp.bfloat16)
    table_low = (remainder - table_middle.astype(jnp.float32)).astype(jnp.bfloat16)
    return (table_high, table_middle, table_low)


def host_tables(group_len, row_count, block_len):
    seq_len = block_len * row_count
    half = group_len // 2 // row_count
    slot = np.arange(group_len)
    freq = (slot // (2 * half)) * half + slot % half
    odd = slot // half % 2 == 1
    nyquist = odd & (freq == 0)
    sine = odd & ~nyquist
    freq = np.where(nyquist, group_len // 2, freq)
    chan = np.arange(group_len)
    angle = 2 * np.pi * (chan[:, None] * freq[None, :] % group_len) / group_len
    chan_table = np.where(sine[None, :], np.sin(angle), np.cos(angle)) / np.sqrt(group_len)
    low = np.arange(block_len)
    angle = 2 * np.pi * (low[:, None] * low[None, :] % block_len) / block_len
    low_table = np.concatenate([np.cos(angle), np.sin(angle)], 1) / np.sqrt(seq_len)
    high = np.arange(row_count)
    angle = 2 * np.pi * (high[:, None] * low[None, :] % seq_len) / seq_len
    return chan_table, low_table, np.cos(angle), np.sin(angle)


def slot_facts(slot, group_len, row_count):
    half = group_len // 2 // row_count
    freq = (slot // (2 * half)) * half + slot % half
    odd = slot // half % 2 == 1
    nyquist = odd & (freq == 0)
    return jnp.where(nyquist, group_len // 2, freq), odd & ~nyquist


def folding(group_len, row_count):
    freq, sine = slot_facts(jnp.arange(group_len, dtype=jnp.int32), group_len, row_count)
    chan = jnp.arange(group_len, dtype=jnp.int32)[None, :]
    direct = chan == freq[:, None]
    mirror = chan == ((group_len - freq) % group_len)[:, None]
    signed = jnp.where(sine[:, None], -1.0, 1.0)
    return jnp.where(direct, signed, jnp.where(mirror, 1.0, 0.0)).astype(jnp.bfloat16)


def on_device_folded(tokens, norm_gain, out_weight):
    row_count = lax.axis_size("row")
    col_count = lax.axis_size("col")
    block_len, group_len = tokens.shape
    full_width = group_len * col_count
    slab = group_len // row_count
    out_width = out_weight.shape[1]
    chan_table, low_table, twist_cos, twist_sin = host_tables(group_len, row_count, block_len)
    chan_table = jnp.asarray(chan_table, jnp.bfloat16)
    low_table = jnp.asarray(low_table, jnp.bfloat16)
    twist_cos = jnp.asarray(twist_cos, jnp.float32)[:, :, None]
    twist_sin = jnp.asarray(twist_sin, jnp.float32)[:, :, None]
    values = tokens.astype(jnp.float32)
    total = lax.psum(jnp.sum(values * values, axis=-1), "col")
    inv_rms = lax.rsqrt(total / full_width + EPSILON)[:, None]
    gain = lax.dynamic_slice_in_dim(norm_gain, lax.axis_index("col") * group_len, group_len)
    normed = (values * inv_rms * gain).astype(jnp.bfloat16)
    chans = jnp.dot(normed, chan_table, preferred_element_type=jnp.float32).astype(jnp.bfloat16)
    moved = lax.all_to_all(chans, "row", split_axis=1, concat_axis=0, tiled=True)
    blocks = moved.reshape(row_count, block_len, slab).astype(jnp.float32)
    _, sine = slot_facts(
        lax.axis_index("row") * slab + jnp.arange(slab, dtype=jnp.int32), group_len, row_count
    )
    tops, bottoms = [], []
    for q in range(row_count):
        real, imag = 0.0, 0.0
        for a in range(row_count):
            angle = 2 * math.pi * (a * q % row_count) / row_count
            real = real + blocks[a] * round(math.cos(angle), 12)
            imag = imag - blocks[a] * round(math.sin(angle), 12)
        turned_real = real * twist_cos[q] + imag * twist_sin[q]
        turned_imag = imag * twist_cos[q] - real * twist_sin[q]
        tops.append(jnp.where(sine, -turned_imag, turned_real).astype(jnp.bfloat16))
        bottoms.append(jnp.where(sine, turned_real, turned_imag).astype(jnp.bfloat16))
    stacked = jnp.concatenate([jnp.concatenate(tops, 1), jnp.concatenate(bottoms, 1)], 0)
    lows = jnp.dot(low_table, stacked, preferred_element_type=jnp.float32).astype(jnp.bfloat16)
    back = lax.all_to_all(
        lows.reshape(row_count, block_len // row_count, row_count * slab),
        "row", split_axis=0, concat_axis=0, tiled=True,
    )
    gathered = lax.all_gather(back, "col", axis=0, tiled=False)
    fold = folding(group_len, row_count)
    folded = jnp.einsum(
        "sm,gme->gse", fold, out_weight.reshape(col_count, group_len, out_width),
        preferred_element_type=jnp.float32,
    ).astype(jnp.bfloat16)
    mapped = jnp.einsum(
        "gspql,gsle->pqe",
        gathered.reshape(col_count, row_count, block_len // row_count, row_count, slab),
        folded.reshape(col_count, row_count, slab, out_width),
        preferred_element_type=jnp.float32,
    )
    return mapped.astype(jnp.bfloat16).reshape(block_len, out_width)


MESH = pl.DeviceIdType.MESH
F32 = jnp.float32
BF16 = jnp.bfloat16
WIDTHS = (16, 32, 32, 16, 16, 16)
NEAR_FIRST = (True, True, True, False, True, True)
FOLDS = (0, 6, 11, 16)
PLAN = (
    "A0", "A1", "I", "A2", "D0", "D1", "F0", "Gn0", "A3", "Gf0", "Gn1", "Xf0", "D2", "Xn1", "Gf1", "Gn2",
    "F1", "A4", "Xn0", "D3", "Xf1", "Xn2", "F2", "Gf2", "A5", "Gn3", "D4", "Xf2", "Mn1", "Gf3", "Mn2", "D5",
    "Xn3", "Gn4", "Xf3", "Gn5", "Mn0", "Gf4", "Xn4", "Mf0", "Mf1", "Gf5", "Mn3", "Xf4", "Xn5", "Mf2", "Mn4",
    "Xf5", "Mf3", "Mf4", "Mn5", "Mf5",
)


def fused_tables(group_len, row_count, block_len):
    seq_len = block_len * row_count
    freqs, sines = [], []
    offset = 0
    for width in WIDTHS:
        half = width // 2
        slot = np.arange(row_count * width)
        freqs.append(row_count // 2 * offset + slot // width * half + slot % half)
        sines.append(slot % width >= half)
        offset += width
    freq, odd = np.concatenate(freqs), np.concatenate(sines)
    nyquist = odd & (freq == 0)
    sine = odd & ~nyquist
    freq = np.where(nyquist, group_len // 2, freq)
    chan = np.arange(group_len)
    angle = 2 * np.pi * (freq[:, None] * chan[None, :] % group_len) / group_len
    chan_table = np.where(sine[:, None], np.sin(angle), np.cos(angle)) / np.sqrt(group_len)
    low = np.arange(block_len)
    angle = 2 * np.pi * (low[:, None] * low[None, :] % block_len) / block_len
    low_table = np.concatenate([np.cos(angle), np.sin(angle)], 0) / np.sqrt(seq_len)
    high = np.arange(row_count)
    angle = 2 * np.pi * (high[:, None] * low[None, :] % seq_len) / seq_len
    return chan_table, low_table, np.concatenate([np.cos(angle), np.sin(angle)], 0)


def fused_kernel(
    dims, x_hbm, gain_hbm, table_hbm, low_hbm, twist_hbm, w_hbm, out_ref,
    x_ref, gain_ref, twist_ref, scaled, table_ref, low_ref, w_ref, fold_ref, folded, send1, recv1, sums, invs, stacked, send2,
    held, lhs, acc,
    l_sem, stay_sem, send_sem, s_recv, i_recv, a_recv, b_recv, g_recv,
):
    row_count, col_count = dims
    block_len, group_len = x_ref.shape
    full_width = group_len * col_count
    out_width = out_ref.shape[2]
    part = block_len // row_count
    slab = group_len // row_count
    chunks = len(WIDTHS)
    offsets = [sum(WIDTHS[:i]) for i in range(chunks)]
    quads = row_count // 2
    r = lax.axis_index("row")
    c = lax.axis_index("col")
    core, inner, side = r % 2, r // 2 % 2, r // 4

    def peer_of(d):
        k = 1 - core if d % 2 else core
        t = 1 - inner if d // 2 % 2 else inner
        s = 1 - side if d // 4 else side
        return 4 * s + 2 * t + k

    x_next = 2 * (c // 2) + 1 - c % 2
    y_next = 2 * (1 - c // 2) + c % 2
    diagonal = 2 * (1 - c // 2) + 1 - c % 2
    col_peers = (x_next, y_next, diagonal)
    near, far = tuple(range(1, quads)), tuple(range(quads, row_count))

    def rows_of(start, size, unit):
        return pl.ds(pl.multiple_of(start, unit), size)

    x_copy = pltpu.make_async_copy(x_hbm, x_ref, l_sem.at[0])
    early = row_count * WIDTHS[0]
    table_copy = pltpu.make_async_copy(table_hbm.at[:early], table_ref.at[:early], l_sem.at[1])
    table_rest = pltpu.make_async_copy(table_hbm.at[early:], table_ref.at[early:], l_sem.at[4])
    low_copy = pltpu.make_async_copy(low_hbm, low_ref, l_sem.at[2])
    w_copy = pltpu.make_async_copy(w_hbm, w_ref, l_sem.at[3])
    gain_copy = pltpu.make_async_copy(
        gain_hbm.at[:, pl.ds(pl.multiple_of(c * group_len, group_len), group_len)], gain_ref, l_sem.at[5]
    )
    twist_copy = pltpu.make_async_copy(twist_hbm, twist_ref, l_sem.at[6])
    for copy in (x_copy, gain_copy, table_copy):
        copy.start()

    barrier = pltpu.get_barrier_semaphore()
    for d in range(1, row_count):
        pl.semaphore_signal(barrier, inc=1, device_id=(peer_of(d), c), device_id_type=MESH)
    for peer in col_peers:
        pl.semaphore_signal(barrier, inc=1, device_id=(r, peer), device_id_type=MESH)

    lanes = (((1,), (1,)), ((), ()))
    x_copy.wait()
    for copy in (table_rest, low_copy, twist_copy, w_copy):
        copy.start()
    gain_copy.wait()
    scaled[...] = (x_ref[...].astype(F32) * gain_ref[...]).astype(BF16)

    def remote(source, target_ref, phase, recv_sem, device):
        pltpu.make_async_remote_copy(
            src_ref=source, dst_ref=target_ref, send_sem=send_sem.at[phase], recv_sem=recv_sem,
            device_id=device, device_id_type=MESH,
        ).start()

    def sent(ref, phase):
        pltpu.make_async_remote_copy(
            src_ref=ref, dst_ref=ref, send_sem=send_sem.at[phase], recv_sem=l_sem.at[0],
            device_id=(peer_of(1), c), device_id_type=MESH,
        ).wait_send()

    def arrived(ref, semaphore):
        pltpu.make_async_remote_copy(
            src_ref=ref, dst_ref=ref, send_sem=l_sem.at[0], recv_sem=semaphore,
            device_id=(peer_of(1), c), device_id_type=MESH,
        ).wait_recv()

    first_stays, second_stays = {}, {}

    def features(i):
        width, offset = WIDTHS[i], offsets[i]
        rows = pl.ds(row_count * offset, row_count * width)
        send1[rows, :] = lax.dot_general(
            table_ref[rows, :], scaled[...], lanes, preferred_element_type=F32
        ).astype(BF16)

    def first_exchange(i):
        width, offset = WIDTHS[i], offsets[i]
        if i == 0:
            square_sums()
            table_copy.wait()
        if i == 1:
            table_rest.wait()
        features(i)
        if i == 0:
            pl.semaphore_wait(barrier, row_count + col_count - 2)
            for peer in col_peers:
                remote(sums.at[c], sums.at[c], 0, s_recv.at[0], (r, peer))
        target = recv1.at[r, pl.ds(offset, width), :]
        for d in far + near[::-1]:
            peer = peer_of(d)
            source = send1.at[rows_of(row_count * offset + peer * width, width, 16), :]
            remote(source, target, 2, a_recv.at[i], (peer, c))
        source = send1.at[rows_of(row_count * offset + r * width, width, 16), :]
        first_stays[i] = pltpu.make_async_copy(source, target, stay_sem.at[0, i])
        first_stays[i].start()

    def square_sums():
        squares = x_ref[...].astype(F32)
        squares = squares * squares
        top = squares.astype(BF16)
        rest = (squares - top.astype(F32)).astype(BF16)
        ones = jnp.ones((16, group_len), BF16)
        own = lax.dot_general(ones, top, lanes, preferred_element_type=F32)
        own = own + lax.dot_general(ones, rest, lanes, preferred_element_type=F32)
        sums[c] = own[:1]

    def inverses():
        arrived(sums.at[: col_count - 1], s_recv.at[0])
        total = sums[0]
        for k in range(1, col_count):
            total = total + sums[k]
        invs[r] = lax.rsqrt(total / full_width + EPSILON)
        for d in far + near[::-1]:
            remote(invs.at[r], invs.at[r], 1, i_recv.at[0], (peer_of(d), c))

    def butterfly(i):
        width, offset = WIDTHS[i], offsets[i]
        half = width // 2
        middle = row_count // 2

        def step(j, carry):
            spot = rows_of(j * 128, 128, 128)
            below = rows_of(block_len + j * 128, 128, 128)
            for base in range(0, width, 16):
                rows = pl.ds(offset + base, 16)
                blocks = [
                    recv1[a, rows, spot].astype(F32) * invs[a, :, spot] for a in range(row_count)
                ]
                even = [blocks[a] + blocks[row_count - a] for a in range(1, middle)]
                odd = [blocks[a] - blocks[row_count - a] for a in range(1, middle)]
                ends = (blocks[0] + blocks[middle], blocks[0] - blocks[middle])
                row = lax.broadcasted_iota(jnp.int32, (16, 128), 0) + base
                sine = row >= half
                if offset == 0:
                    sine = (row > half) | ((row == half) & (r > 0))
                plain = base + 16 <= half
                turned = base >= half and (offset > 0 or base > half)
                for q in range(middle + 1):
                    real = ends[q % 2]
                    imag = None
                    for a in range(1, middle):
                        angle = 2 * math.pi * (a * q % row_count) / row_count
                        cosine, sinus = round(math.cos(angle), 12), round(math.sin(angle), 12)
                        if cosine:
                            real = real + (even[a - 1] if cosine == 1 else even[a - 1] * cosine)
                        if sinus:
                            term = odd[a - 1] * -sinus
                            imag = term if imag is None else imag + term
                    for k, sign in ((q, 1.0), (row_count - q, -1.0)):
                        if k == row_count or (sign < 0 and k == q):
                            continue
                        if k == 0:
                            turned_real, turned_imag = real, jnp.zeros_like(real)
                        else:
                            cosine = twist_ref[k : k + 1, spot]
                            sinus = twist_ref[row_count + k : row_count + k + 1, spot]
                            if imag is None:
                                turned_real, turned_imag = real * cosine, -(real * sinus)
                            elif sign > 0:
                                turned_real = real * cosine + imag * sinus
                                turned_imag = imag * cosine - real * sinus
                            else:
                                turned_real = real * cosine - imag * sinus
                                turned_imag = -(imag * cosine + real * sinus)
                        if plain:
                            upper, lower = turned_real, turned_imag
                        elif turned:
                            upper, lower = -turned_imag, turned_real
                        else:
                            upper = jnp.where(sine, -turned_imag, turned_real)
                            lower = jnp.where(sine, turned_real, turned_imag)
                        place = pl.ds((k % 2 * quads + k // 2) * width + base, 16)
                        stacked[place, spot] = upper.astype(BF16)
                        stacked[place, below] = lower.astype(BF16)
            return carry

        lax.fori_loop(0, block_len // 128, step, 0)

    def second_exchange(i):
        width, offset = WIDTHS[i], offsets[i]
        lane = lax.broadcasted_iota(jnp.int32, (quads * width, 128), 1)
        first_half = lane < part
        target = held.at[c, :, rows_of(row_count * offset + r * width, width, 16), :]
        for nearby in (True, False) if NEAR_FIRST[i] else (False, True):
            where = side if nearby else 1 - side
            lows = jnp.dot(
                stacked[: row_count * width, :],
                low_ref[:, rows_of(where * (block_len // 2), block_len // 2, 256)],
                preferred_element_type=F32,
            )
            for t in range(2):
                left = lows[: quads * width, t * 128 : (t + 1) * 128]
                right = lows[quads * width :, t * 128 : (t + 1) * 128]
                pair = (
                    jnp.where(first_half, left, pltpu.roll(right, part, 1)),
                    jnp.where(first_half, pltpu.roll(left, part, 1), right),
                )
                for k in range(2):
                    value = pair[k].astype(BF16).reshape(quads, width, 128)
                    send2[4 * where + 2 * t + k, :, pl.ds(offset, width), :] = value
            for d in near[::-1] if nearby else far:
                peer = peer_of(d)
                source = send2.at[peer, :, pl.ds(offset, width), :]
                remote(source, target, 3, b_recv.at[i, 0 if nearby else 1], (peer, c))
        source = send2.at[r, :, pl.ds(offset, width), :]
        second_stays[i] = pltpu.make_async_copy(source, target, stay_sem.at[1, i])
        second_stays[i].start()

    def transform(i):
        width, offset = WIDTHS[i], offsets[i]
        first_stays[i].wait()
        if i == 0:
            low_copy.wait()
            twist_copy.wait()
            arrived(invs.at[: row_count - 1], i_recv.at[0])
        arrived(recv1.at[: row_count - 1, pl.ds(offset, width), :], a_recv.at[i])
        butterfly(i)
        second_exchange(i)

    def place_of(i, h):
        width, offset = WIDTHS[i], offsets[i]
        where = side if h == "n" else 1 - side
        return rows_of(row_count * offset + where * quads * width, quads * width, 16)

    def piece(origin, i, h, u):
        return held.at[origin, pl.ds(2 * u, 2), place_of(i, h), :]

    def spread(i, h, u, origin, target, kind):
        slot = 2 * i + (h == "f")
        part_ref = piece(origin, i, h, u)
        remote(part_ref, part_ref, 4, g_recv.at[slot, kind], (r, target))

    def came(i, h, u, origin, kind):
        arrived(piece(origin, i, h, u), g_recv.at[2 * i + (h == "f"), kind])

    def gather(i, h):
        width, offset = WIDTHS[i], offsets[i]
        if h == "n":
            arrived(held.at[c, :, pl.ds(row_count * offset, len(near) * width), :], b_recv.at[i, 0])
            second_stays[i].wait()
        else:
            arrived(held.at[c, :, pl.ds(row_count * offset, len(far) * width), :], b_recv.at[i, 1])
        spread(i, h, 0, c, x_next, 0)
        spread(i, h, 1, c, y_next, 1)
        spread(i, h, 1, c, x_next, 2)
        spread(i, h, 0, c, y_next, 2)

    def forward(i, h):
        came(i, h, 0, x_next, 0)
        spread(i, h, 0, x_next, y_next, 2)
        came(i, h, 1, y_next, 1)
        spread(i, h, 1, y_next, x_next, 2)

    wide, broad = 256, 512
    pieces = out_width // wide

    def fold_spans(i):
        width, offset = WIDTHS[i], offsets[i]
        start, count = quads * offset, quads * width
        high = min(group_len - start - count, group_len - count - 16)
        return start, count, high, 2 * count + 16 + (16 if i == 0 else 0)

    def fold_matrix(i):
        width = WIDTHS[i]
        start, count, high, depth = fold_spans(i)
        shape = (2 * count, depth)
        slot = lax.broadcasted_iota(jnp.int32, shape, 0)
        column = lax.broadcasted_iota(jnp.int32, shape, 1)
        half = width // 2
        freq = start + slot // width * half + slot % half
        odd = slot % width >= half
        nyquist = odd & (freq == 0)
        direct = (column == freq - start) & ~nyquist & (column < count)
        mirror = (column - count + high == group_len - freq) & (freq > 0)
        mirror = mirror & (column >= count) & (column < 2 * count + 16)
        middle = nyquist & (column == 2 * count + 16)
        signed = jnp.where(odd, -1.0, 1.0)
        matrix = jnp.where(direct, signed, jnp.where(mirror | middle, 1.0, 0.0)).astype(BF16)
        fold_ref[row_count * offsets[i] : row_count * (offsets[i] + width), :depth] = matrix

    def fold(m):
        if m == 0:
            for i in range(chunks):
                fold_matrix(i)
            w_copy.wait()

        def step(n, carry):
            group = n // pieces
            origin = group * group_len
            cols = rows_of(n % pieces * wide, wide, wide)
            for i in range(chunks):
                start, count, high, depth = fold_spans(i)
                base = row_count * offsets[i]
                taken = [w_ref[rows_of(origin + start, count, 16), cols]]
                taken.append(w_ref[rows_of(origin + high, count + 16, 16), cols])
                if i == 0:
                    taken.append(w_ref[rows_of(origin + group_len // 2, 16, 16), cols])
                value = jnp.dot(
                    fold_ref[base : base + 2 * count, :depth], jnp.concatenate(taken, 0),
                    preferred_element_type=F32,
                ).astype(BF16)
                for s in range(2):
                    start = base * col_count + s * col_count * count + group * count
                    folded[rows_of(start, count, 16), cols] = value[s * count : (s + 1) * count]
            return carry

        lax.fori_loop(FOLDS[m], FOLDS[m + 1], step, 0)

    done = []

    def multiply(i, h):
        width, offset = WIDTHS[i], offsets[i]
        count = quads * width
        depth = col_count * count
        arrived(held.at[:2, :, place_of(i, h), :], g_recv.at[2 * i + (h == "f"), 2])
        for g in range(col_count):
            for q in range(quads):
                lhs[q * 128 : (q + 1) * 128, g * count : (g + 1) * count] = jnp.transpose(
                    held[g, q, place_of(i, h), :]
                )
        where = side if h == "n" else 1 - side
        rows = rows_of(row_count * offset * col_count + where * depth, depth, 16)
        first, last = not done, len(done) == 2 * chunks - 1
        done.append((i, h))

        def step(n, carry):
            cols = rows_of(n * broad, broad, broad)
            value = jnp.dot(lhs[:, :depth], folded[rows, cols], preferred_element_type=F32)
            if not first:
                value = acc[:, cols] + value
            if not last:
                acc[:, cols] = value
            else:
                out_ref[:, :, cols] = value.astype(BF16).reshape(row_count, part, broad)
            return carry

        lax.fori_loop(0, out_width // broad, step, 0)

    for token in PLAN:
        i = int(token[-1]) if token[-1].isdigit() else 0
        with jax.named_scope(token):
            match token[0]:
                case "A":
                    first_exchange(i)
                case "I":
                    inverses()
                case "F":
                    fold(i)
                case "D":
                    transform(i)
                case "G":
                    gather(i, token[1])
                case "X":
                    forward(i, token[1])
                case "M":
                    multiply(i, token[1])

    sent(sums.at[: col_count - 1], 0)
    sent(invs.at[: row_count - 1], 1)
    sent(send1.at[: group_len - slab], 2)
    sent(send2.at[: row_count - 1], 3)
    sent(held.at[: col_count - 1], 4)


def on_device_fused(tokens, norm_gain, out_weight):
    row_count = lax.axis_size("row")
    col_count = lax.axis_size("col")
    block_len, group_len = tokens.shape
    out_width = out_weight.shape[1]
    slab = group_len // row_count
    part = block_len // row_count
    chunks = len(WIDTHS)
    widest = max(WIDTHS)
    chan_table, low_table, twist = fused_tables(group_len, row_count, block_len)
    vmem = pl.BlockSpec(memory_space=pltpu.VMEM)
    hbm = pl.BlockSpec(memory_space=pl.ANY)
    dma = pltpu.SemaphoreType.DMA
    mapped = pl.pallas_call(
        functools.partial(fused_kernel, (row_count, col_count)),
        out_shape=pltpu.VMEM((row_count, part, out_width), BF16),
        in_specs=[hbm] * 6,
        out_specs=vmem,
        scratch_shapes=[
            pltpu.VMEM((block_len, group_len), BF16),
            pltpu.VMEM((1, group_len), F32),
            pltpu.VMEM(twist.shape, F32),
            pltpu.VMEM((block_len, group_len), BF16),
            pltpu.VMEM(chan_table.shape, BF16),
            pltpu.VMEM(low_table.shape, BF16),
            pltpu.VMEM(out_weight.shape, BF16),
            pltpu.VMEM((group_len, row_count * widest + 32), BF16),
            pltpu.VMEM(out_weight.shape, BF16),
            pltpu.VMEM((group_len, block_len), BF16),
            pltpu.VMEM((row_count, slab, block_len), BF16),
            pltpu.VMEM((col_count, 1, block_len), F32),
            pltpu.VMEM((row_count, 1, block_len), F32),
            pltpu.VMEM((row_count * widest, 2 * block_len), BF16),
            pltpu.VMEM((row_count, row_count // 2, slab, 128), BF16),
            pltpu.VMEM((col_count, row_count // 2, group_len, 128), BF16),
            pltpu.VMEM((block_len, col_count * row_count // 2 * widest), BF16),
            pltpu.VMEM((block_len, out_width), F32),
            dma((7,)), dma((2, chunks)), dma((5,)), dma((1,)), dma((1,)),
            dma((chunks,)), dma((chunks, 2)), dma((2 * chunks, 3)),
        ],
        compiler_params=pltpu.CompilerParams(
            collective_id=0, has_side_effects=True, vmem_limit_bytes=60 * 1024 * 1024
        ),
    )(
        tokens, norm_gain[None, :], jnp.asarray(chan_table, BF16), jnp.asarray(low_table, BF16),
        jnp.asarray(twist, F32), out_weight,
    )
    return jnp.transpose(mapped, (1, 0, 2)).reshape(block_len, out_width)


def on_device(tokens, norm_gain, out_weight):
    row_count = lax.axis_size("row")
    col_count = lax.axis_size("col")
    block_len, local_width = tokens.shape
    full_width = local_width * col_count
    group_len = full_width // GROUPS
    share_len = block_len // col_count
    seq_len = block_len * row_count
    slab_len = full_width // row_count
    col_index = lax.axis_index("col")
    chan_idx = jnp.arange(group_len, dtype=jnp.int32)
    cosines, sines = phases(chan_idx, chan_idx, group_len)
    chan_table = jnp.concatenate([cosines, sines], axis=1) / math.sqrt(group_len)
    table_parts = split_table(chan_table)
    arranged = tokens.reshape(col_count, share_len, local_width)
    portion = lax.all_to_all(arranged, "col", split_axis=0, concat_axis=2, tiled=True)
    item_count = portion.shape[1]
    values = portion.astype(jnp.float32)
    inv_rms = lax.rsqrt(jnp.mean(values * values, axis=-1, keepdims=True) + EPSILON)
    normed = lax.optimization_barrier((values * inv_rms * norm_gain).astype(jnp.bfloat16))
    grouped = normed.reshape(item_count, GROUPS, group_len)
    result = jnp.einsum("pgm,mj->pgj", grouped, table_parts[0], preferred_element_type=jnp.float32)
    result = result + jnp.einsum(
        "pgm,mj->pgj", grouped, table_parts[1], preferred_element_type=jnp.float32
    )
    result = result + jnp.einsum(
        "pgm,mj->pgj", grouped, table_parts[2], preferred_element_type=jnp.float32
    )
    high_idx = jnp.arange(row_count, dtype=jnp.int32)
    high_cos, high_sin = phases(high_idx, high_idx, row_count)
    high_table = jnp.concatenate(
        [jnp.concatenate([high_cos, -high_sin], 1), jnp.concatenate([-high_sin, -high_cos], 1)], 0
    )
    parts = (
        lax.all_to_all(
            result[..., :group_len].reshape(1, item_count, full_width),
            "row",
            split_axis=2,
            concat_axis=0,
            tiled=True,
        ),
        lax.all_to_all(
            result[..., group_len:].reshape(1, item_count, full_width),
            "row",
            split_axis=2,
            concat_axis=0,
            tiled=True,
        ),
    )
    item_count = parts[0].shape[1]
    stacked = jnp.concatenate(parts, 0).reshape(2 * row_count, item_count * slab_len)
    result = jnp.dot(high_table, stacked, precision=PRECISE)
    real_part = result[:row_count].reshape(row_count, item_count, slab_len)
    imag_part = result[row_count:].reshape(row_count, item_count, slab_len)
    local_pos = col_index * share_len + jnp.arange(share_len, dtype=jnp.int32)
    twist_cos, twist_sin = phases(high_idx, local_pos, seq_len)
    twist_cos = twist_cos[:, :, None]
    twist_sin = twist_sin[:, :, None]
    turned_real = real_part * twist_cos + imag_part * twist_sin
    turned_imag = imag_part * twist_cos - real_part * twist_sin
    low_idx = jnp.arange(block_len, dtype=jnp.int32)
    low_cos, low_sin = phases(low_idx, low_idx, block_len)
    low_cos = low_cos / math.sqrt(seq_len)
    low_sin = low_sin / math.sqrt(seq_len)
    low_table = jnp.concatenate([low_cos, low_sin], 1)
    stacked = jnp.concatenate(
        (
            lax.all_to_all(turned_real, "col", split_axis=0, concat_axis=1, tiled=True),
            lax.all_to_all(turned_imag, "col", split_axis=0, concat_axis=1, tiled=True),
        ),
        1,
    )
    finished = (jnp.einsum("ks,asc->akc", low_table, stacked, precision=PRECISE),)[0]
    spectrum = finished.astype(jnp.bfloat16)
    returned = lax.all_to_all(spectrum, "row", split_axis=1, concat_axis=2, tiled=True)
    mapped = jnp.einsum(
        "akd,de->kae",
        lax.all_gather(returned, "col", axis=0, tiled=True),
        out_weight,
        preferred_element_type=jnp.float32,
    )
    return mapped.astype(jnp.bfloat16).reshape(block_len, local_width)


def solution(mesh):
    def body(tokens, norm_gain, out_weight):
        whole_groups = tokens.shape[1] * GROUPS == out_weight.shape[0]
        slab = tokens.shape[1] // mesh.shape["row"]
        program = on_device_folded if whole_groups else on_device
        if whole_groups and slab == 128 and mesh.shape["col"] == 4 and mesh.shape["row"] == 8:
            program = on_device_fused
        return program(tokens, norm_gain, out_weight)

    placed = (P("row", "col"), P(), P(None, "col"))
    return jax.shard_map(
        body, mesh=mesh, in_specs=placed, out_specs=P("row", "col"), check_vma=False
    )
```

```python
import functools
import math

import numpy as np

import jax
import jax.numpy as jnp
from jax import lax
from jax.experimental import pallas as pl
from jax.experimental.pallas import tpu as pltpu
from jax.sharding import PartitionSpec as P

GROUPS = 4


EPSILON = 1e-06
PRECISE = lax.Precision.HIGHEST


def phases(left_idx, right_idx, period):
    product = left_idx[:, None] * right_idx[None, :] % period
    angles = product.astype(jnp.float32) * (2.0 * math.pi / period)
    return (jnp.cos(angles), jnp.sin(angles))


def split_table(table):
    table_high = table.astype(jnp.bfloat16)
    remainder = table - table_high.astype(jnp.float32)
    table_middle = remainder.astype(jnp.bfloat16)
    table_low = (remainder - table_middle.astype(jnp.float32)).astype(jnp.bfloat16)
    return (table_high, table_middle, table_low)


def host_tables(group_len, row_count, block_len):
    seq_len = block_len * row_count
    half = group_len // 2 // row_count
    slot = np.arange(group_len)
    freq = (slot // (2 * half)) * half + slot % half
    odd = slot // half % 2 == 1
    nyquist = odd & (freq == 0)
    sine = odd & ~nyquist
    freq = np.where(nyquist, group_len // 2, freq)
    chan = np.arange(group_len)
    angle = 2 * np.pi * (chan[:, None] * freq[None, :] % group_len) / group_len
    chan_table = np.where(sine[None, :], np.sin(angle), np.cos(angle)) / np.sqrt(group_len)
    low = np.arange(block_len)
    angle = 2 * np.pi * (low[:, None] * low[None, :] % block_len) / block_len
    low_table = np.concatenate([np.cos(angle), np.sin(angle)], 1) / np.sqrt(seq_len)
    high = np.arange(row_count)
    angle = 2 * np.pi * (high[:, None] * low[None, :] % seq_len) / seq_len
    return chan_table, low_table, np.cos(angle), np.sin(angle)


def slot_facts(slot, group_len, row_count):
    half = group_len // 2 // row_count
    freq = (slot // (2 * half)) * half + slot % half
    odd = slot // half % 2 == 1
    nyquist = odd & (freq == 0)
    return jnp.where(nyquist, group_len // 2, freq), odd & ~nyquist


def folding(group_len, row_count):
    freq, sine = slot_facts(jnp.arange(group_len, dtype=jnp.int32), group_len, row_count)
    chan = jnp.arange(group_len, dtype=jnp.int32)[None, :]
    direct = chan == freq[:, None]
    mirror = chan == ((group_len - freq) % group_len)[:, None]
    signed = jnp.where(sine[:, None], -1.0, 1.0)
    return jnp.where(direct, signed, jnp.where(mirror, 1.0, 0.0)).astype(jnp.bfloat16)


def on_device_folded(tokens, norm_gain, out_weight):
    row_count = lax.axis_size("row")
    col_count = lax.axis_size("col")
    block_len, group_len = tokens.shape
    full_width = group_len * col_count
    slab = group_len // row_count
    out_width = out_weight.shape[1]
    chan_table, low_table, twist_cos, twist_sin = host_tables(group_len, row_count, block_len)
    chan_table = jnp.asarray(chan_table, jnp.bfloat16)
    low_table = jnp.asarray(low_table, jnp.bfloat16)
    twist_cos = jnp.asarray(twist_cos, jnp.float32)[:, :, None]
    twist_sin = jnp.asarray(twist_sin, jnp.float32)[:, :, None]
    values = tokens.astype(jnp.float32)
    total = lax.psum(jnp.sum(values * values, axis=-1), "col")
    inv_rms = lax.rsqrt(total / full_width + EPSILON)[:, None]
    gain = lax.dynamic_slice_in_dim(norm_gain, lax.axis_index("col") * group_len, group_len)
    normed = (values * inv_rms * gain).astype(jnp.bfloat16)
    chans = jnp.dot(normed, chan_table, preferred_element_type=jnp.float32).astype(jnp.bfloat16)
    moved = lax.all_to_all(chans, "row", split_axis=1, concat_axis=0, tiled=True)
    blocks = moved.reshape(row_count, block_len, slab).astype(jnp.float32)
    _, sine = slot_facts(
        lax.axis_index("row") * slab + jnp.arange(slab, dtype=jnp.int32), group_len, row_count
    )
    tops, bottoms = [], []
    for q in range(row_count):
        real, imag = 0.0, 0.0
        for a in range(row_count):
            angle = 2 * math.pi * (a * q % row_count) / row_count
            real = real + blocks[a] * round(math.cos(angle), 12)
            imag = imag - blocks[a] * round(math.sin(angle), 12)
        turned_real = real * twist_cos[q] + imag * twist_sin[q]
        turned_imag = imag * twist_cos[q] - real * twist_sin[q]
        tops.append(jnp.where(sine, -turned_imag, turned_real).astype(jnp.bfloat16))
        bottoms.append(jnp.where(sine, turned_real, turned_imag).astype(jnp.bfloat16))
    stacked = jnp.concatenate([jnp.concatenate(tops, 1), jnp.concatenate(bottoms, 1)], 0)
    lows = jnp.dot(low_table, stacked, preferred_element_type=jnp.float32).astype(jnp.bfloat16)
    back = lax.all_to_all(
        lows.reshape(row_count, block_len // row_count, row_count * slab),
        "row", split_axis=0, concat_axis=0, tiled=True,
    )
    gathered = lax.all_gather(back, "col", axis=0, tiled=False)
    fold = folding(group_len, row_count)
    folded = jnp.einsum(
        "sm,gme->gse", fold, out_weight.reshape(col_count, group_len, out_width),
        preferred_element_type=jnp.float32,
    ).astype(jnp.bfloat16)
    mapped = jnp.einsum(
        "gspql,gsle->pqe",
        gathered.reshape(col_count, row_count, block_len // row_count, row_count, slab),
        folded.reshape(col_count, row_count, slab, out_width),
        preferred_element_type=jnp.float32,
    )
    return mapped.astype(jnp.bfloat16).reshape(block_len, out_width)


MESH = pl.DeviceIdType.MESH
F32 = jnp.float32
BF16 = jnp.bfloat16
WIDTHS = (16, 32, 32, 16, 16, 16)
NEAR_FIRST = (True, True, True, False, True, True)
FOLDS = (0, 6, 11, 16)
PLAN = (
    "A0", "A1", "I", "A2", "D0", "D1", "F0", "Gn0", "A3", "Gf0", "Gn1", "Xf0", "D2", "Xn1", "Gf1", "Gn2",
    "F1", "A4", "Xn0", "D3", "Xf1", "Xn2", "F2", "Gf2", "A5", "Gn3", "D4", "Xf2", "Mn1", "Gf3", "Mn2", "D5",
    "Xn3", "Gn4", "Xf3", "Gn5", "Mn0", "Gf4", "Xn4", "Mf0", "Mf1", "Gf5", "Mn3", "Xf4", "Xn5", "Mf2", "Mn4",
    "Xf5", "Mf3", "Mf4", "Mn5", "Mf5",
)


def fused_tables(group_len, row_count, block_len):
    seq_len = block_len * row_count
    freqs, sines = [], []
    offset = 0
    for width in WIDTHS:
        half = width // 2
        slot = np.arange(row_count * width)
        freqs.append(row_count // 2 * offset + slot // width * half + slot % half)
        sines.append(slot % width >= half)
        offset += width
    freq, odd = np.concatenate(freqs), np.concatenate(sines)
    nyquist = odd & (freq == 0)
    sine = odd & ~nyquist
    freq = np.where(nyquist, group_len // 2, freq)
    chan = np.arange(group_len)
    angle = 2 * np.pi * (freq[:, None] * chan[None, :] % group_len) / group_len
    chan_table = np.where(sine[:, None], np.sin(angle), np.cos(angle)) / np.sqrt(group_len)
    low = np.arange(block_len)
    angle = 2 * np.pi * (low[:, None] * low[None, :] % block_len) / block_len
    low_table = np.concatenate([np.cos(angle), np.sin(angle)], 0) / np.sqrt(seq_len)
    high = np.arange(row_count)
    angle = 2 * np.pi * (high[:, None] * low[None, :] % seq_len) / seq_len
    return chan_table, low_table, np.concatenate([np.cos(angle), np.sin(angle)], 0)


def fused_kernel(
    dims, x_hbm, gain_hbm, table_hbm, low_hbm, twist_hbm, w_hbm, out_ref,
    x_ref, gain_ref, twist_ref, scaled, table_ref, low_ref, w_ref, fold_ref, folded, send1, recv1, sums, invs, stacked, send2,
    held, lhs, acc,
    l_sem, stay_sem, send_sem, s_recv, i_recv, a_recv, b_recv, g_recv,
):
    row_count, col_count = dims
    block_len, group_len = x_ref.shape
    full_width = group_len * col_count
    out_width = out_ref.shape[2]
    part = block_len // row_count
    slab = group_len // row_count
    chunks = len(WIDTHS)
    offsets = [sum(WIDTHS[:i]) for i in range(chunks)]
    quads = row_count // 2
    r = lax.axis_index("row")
    c = lax.axis_index("col")
    core, inner, side = r % 2, r // 2 % 2, r // 4

    def peer_of(d):
        k = 1 - core if d % 2 else core
        t = 1 - inner if d // 2 % 2 else inner
        s = 1 - side if d // 4 else side
        return 4 * s + 2 * t + k

    x_next = 2 * (c // 2) + 1 - c % 2
    y_next = 2 * (1 - c // 2) + c % 2
    diagonal = 2 * (1 - c // 2) + 1 - c % 2
    col_peers = (x_next, y_next, diagonal)
    near, far = tuple(range(1, quads)), tuple(range(quads, row_count))

    def rows_of(start, size, unit):
        return pl.ds(pl.multiple_of(start, unit), size)

    x_copy = pltpu.make_async_copy(x_hbm, x_ref, l_sem.at[0])
    early = row_count * WIDTHS[0]
    table_copy = pltpu.make_async_copy(table_hbm.at[:early], table_ref.at[:early], l_sem.at[1])
    table_rest = pltpu.make_async_copy(table_hbm.at[early:], table_ref.at[early:], l_sem.at[4])
    low_copy = pltpu.make_async_copy(low_hbm, low_ref, l_sem.at[2])
    w_copy = pltpu.make_async_copy(w_hbm, w_ref, l_sem.at[3])
    gain_copy = pltpu.make_async_copy(
        gain_hbm.at[:, pl.ds(pl.multiple_of(c * group_len, group_len), group_len)], gain_ref, l_sem.at[5]
    )
    twist_copy = pltpu.make_async_copy(twist_hbm, twist_ref, l_sem.at[6])
    for copy in (x_copy, gain_copy, table_copy):
        copy.start()

    barrier = pltpu.get_barrier_semaphore()
    for d in range(1, row_count):
        pl.semaphore_signal(barrier, inc=1, device_id=(peer_of(d), c), device_id_type=MESH)
    for peer in col_peers:
        pl.semaphore_signal(barrier, inc=1, device_id=(r, peer), device_id_type=MESH)

    lanes = (((1,), (1,)), ((), ()))
    x_copy.wait()
    for copy in (table_rest, low_copy, twist_copy, w_copy):
        copy.start()
    gain_copy.wait()
    scaled[...] = (x_ref[...].astype(F32) * gain_ref[...]).astype(BF16)

    def remote(source, target_ref, phase, recv_sem, device):
        pltpu.make_async_remote_copy(
            src_ref=source, dst_ref=target_ref, send_sem=send_sem.at[phase], recv_sem=recv_sem,
            device_id=device, device_id_type=MESH,
        ).start()

    def sent(ref, phase):
        pltpu.make_async_remote_copy(
            src_ref=ref, dst_ref=ref, send_sem=send_sem.at[phase], recv_sem=l_sem.at[0],
            device_id=(peer_of(1), c), device_id_type=MESH,
        ).wait_send()

    def arrived(ref, semaphore):
        pltpu.make_async_remote_copy(
            src_ref=ref, dst_ref=ref, send_sem=l_sem.at[0], recv_sem=semaphore,
            device_id=(peer_of(1), c), device_id_type=MESH,
        ).wait_recv()

    first_stays, second_stays = {}, {}

    def features(i):
        width, offset = WIDTHS[i], offsets[i]
        rows = pl.ds(row_count * offset, row_count * width)
        send1[rows, :] = lax.dot_general(
            table_ref[rows, :], scaled[...], lanes, preferred_element_type=F32
        ).astype(BF16)

    def first_exchange(i):
        width, offset = WIDTHS[i], offsets[i]
        if i == 0:
            table_copy.wait()
        if i == 1:
            table_rest.wait()
        features(i)
        if i == 0:
            pl.semaphore_wait(barrier, row_count + col_count - 2)
        target = recv1.at[r, pl.ds(offset, width), :]
        for d in far + near[::-1]:
            peer = peer_of(d)
            source = send1.at[rows_of(row_count * offset + peer * width, width, 16), :]
            remote(source, target, 2, a_recv.at[i], (peer, c))
        source = send1.at[rows_of(row_count * offset + r * width, width, 16), :]
        first_stays[i] = pltpu.make_async_copy(source, target, stay_sem.at[0, i])
        first_stays[i].start()
        if i == 0:
            square_sums()
            for peer in col_peers:
                remote(sums.at[c], sums.at[c], 0, s_recv.at[0], (r, peer))

    def square_sums():
        squares = x_ref[...].astype(F32)
        squares = squares * squares
        top = squares.astype(BF16)
        rest = (squares - top.astype(F32)).astype(BF16)
        ones = jnp.ones((16, group_len), BF16)
        own = lax.dot_general(ones, top, lanes, preferred_element_type=F32)
        own = own + lax.dot_general(ones, rest, lanes, preferred_element_type=F32)
        sums[c] = own[:1]

    def inverses():
        arrived(sums.at[: col_count - 1], s_recv.at[0])
        total = sums[0]
        for k in range(1, col_count):
            total = total + sums[k]
        invs[r] = lax.rsqrt(total / full_width + EPSILON)
        for d in far + near[::-1]:
            remote(invs.at[r], invs.at[r], 1, i_recv.at[0], (peer_of(d), c))

    def butterfly(i):
        width, offset = WIDTHS[i], offsets[i]
        half = width // 2
        middle = row_count // 2

        def step(j, carry):
            spot = rows_of(j * 128, 128, 128)
            below = rows_of(block_len + j * 128, 128, 128)
            for base in range(0, width, 16):
                rows = pl.ds(offset + base, 16)
                blocks = [
                    recv1[a, rows, spot].astype(F32) * invs[a, :, spot] for a in range(row_count)
                ]
                even = [blocks[a] + blocks[row_count - a] for a in range(1, middle)]
                odd = [blocks[a] - blocks[row_count - a] for a in range(1, middle)]
                ends = (blocks[0] + blocks[middle], blocks[0] - blocks[middle])
                row = lax.broadcasted_iota(jnp.int32, (16, 128), 0) + base
                sine = row >= half
                if offset == 0:
                    sine = (row > half) | ((row == half) & (r > 0))
                plain = base + 16 <= half
                turned = base >= half and (offset > 0 or base > half)
                for q in range(middle + 1):
                    real = ends[q % 2]
                    imag = None
                    for a in range(1, middle):
                        angle = 2 * math.pi * (a * q % row_count) / row_count
                        cosine, sinus = round(math.cos(angle), 12), round(math.sin(angle), 12)
                        if cosine:
                            real = real + (even[a - 1] if cosine == 1 else even[a - 1] * cosine)
                        if sinus:
                            term = odd[a - 1] * -sinus
                            imag = term if imag is None else imag + term
                    for k, sign in ((q, 1.0), (row_count - q, -1.0)):
                        if k == row_count or (sign < 0 and k == q):
                            continue
                        if k == 0:
                            turned_real, turned_imag = real, jnp.zeros_like(real)
                        else:
                            cosine = twist_ref[k : k + 1, spot]
                            sinus = twist_ref[row_count + k : row_count + k + 1, spot]
                            if imag is None:
                                turned_real, turned_imag = real * cosine, -(real * sinus)
                            elif sign > 0:
                                turned_real = real * cosine + imag * sinus
                                turned_imag = imag * cosine - real * sinus
                            else:
                                turned_real = real * cosine - imag * sinus
                                turned_imag = -(imag * cosine + real * sinus)
                        if plain:
                            upper, lower = turned_real, turned_imag
                        elif turned:
                            upper, lower = -turned_imag, turned_real
                        else:
                            upper = jnp.where(sine, -turned_imag, turned_real)
                            lower = jnp.where(sine, turned_real, turned_imag)
                        place = pl.ds((k % 2 * quads + k // 2) * width + base, 16)
                        stacked[place, spot] = upper.astype(BF16)
                        stacked[place, below] = lower.astype(BF16)
            return carry

        lax.fori_loop(0, block_len // 128, step, 0)

    def second_exchange(i):
        width, offset = WIDTHS[i], offsets[i]
        lane = lax.broadcasted_iota(jnp.int32, (quads * width, 128), 1)
        first_half = lane < part
        target = held.at[c, :, rows_of(row_count * offset + r * width, width, 16), :]
        for nearby in (True, False) if NEAR_FIRST[i] else (False, True):
            where = side if nearby else 1 - side
            lows = jnp.dot(
                stacked[: row_count * width, :],
                low_ref[:, rows_of(where * (block_len // 2), block_len // 2, 256)],
                preferred_element_type=F32,
            )
            for t in range(2):
                left = lows[: quads * width, t * 128 : (t + 1) * 128]
                right = lows[quads * width :, t * 128 : (t + 1) * 128]
                pair = (
                    jnp.where(first_half, left, pltpu.roll(right, part, 1)),
                    jnp.where(first_half, pltpu.roll(left, part, 1), right),
                )
                for k in range(2):
                    value = pair[k].astype(BF16).reshape(quads, width, 128)
                    send2[4 * where + 2 * t + k, :, pl.ds(offset, width), :] = value
            for d in near[::-1] if nearby else far:
                peer = peer_of(d)
                source = send2.at[peer, :, pl.ds(offset, width), :]
                remote(source, target, 3, b_recv.at[i, 0 if nearby else 1], (peer, c))
        source = send2.at[r, :, pl.ds(offset, width), :]
        second_stays[i] = pltpu.make_async_copy(source, target, stay_sem.at[1, i])
        second_stays[i].start()

    def transform(i):
        width, offset = WIDTHS[i], offsets[i]
        first_stays[i].wait()
        if i == 0:
            low_copy.wait()
            twist_copy.wait()
            arrived(invs.at[: row_count - 1], i_recv.at[0])
        arrived(recv1.at[: row_count - 1, pl.ds(offset, width), :], a_recv.at[i])
        butterfly(i)
        second_exchange(i)

    def place_of(i, h):
        width, offset = WIDTHS[i], offsets[i]
        where = side if h == "n" else 1 - side
        return rows_of(row_count * offset + where * quads * width, quads * width, 16)

    def piece(origin, i, h, u):
        return held.at[origin, pl.ds(2 * u, 2), place_of(i, h), :]

    def spread(i, h, u, origin, target, kind):
        slot = 2 * i + (h == "f")
        part_ref = piece(origin, i, h, u)
        remote(part_ref, part_ref, 4, g_recv.at[slot, kind], (r, target))

    def came(i, h, u, origin, kind):
        arrived(piece(origin, i, h, u), g_recv.at[2 * i + (h == "f"), kind])

    def gather(i, h):
        width, offset = WIDTHS[i], offsets[i]
        if h == "n":
            arrived(held.at[c, :, pl.ds(row_count * offset, len(near) * width), :], b_recv.at[i, 0])
            second_stays[i].wait()
        else:
            arrived(held.at[c, :, pl.ds(row_count * offset, len(far) * width), :], b_recv.at[i, 1])
        spread(i, h, 0, c, x_next, 0)
        spread(i, h, 1, c, y_next, 1)
        spread(i, h, 1, c, x_next, 2)
        spread(i, h, 0, c, y_next, 2)

    def forward(i, h):
        came(i, h, 0, x_next, 0)
        spread(i, h, 0, x_next, y_next, 2)
        came(i, h, 1, y_next, 1)
        spread(i, h, 1, y_next, x_next, 2)

    wide, broad = 256, 512
    pieces = out_width // wide

    def fold_spans(i):
        width, offset = WIDTHS[i], offsets[i]
        start, count = quads * offset, quads * width
        high = min(group_len - start - count, group_len - count - 16)
        return start, count, high, 2 * count + 16 + (16 if i == 0 else 0)

    def fold_matrix(i):
        width = WIDTHS[i]
        start, count, high, depth = fold_spans(i)
        shape = (2 * count, depth)
        slot = lax.broadcasted_iota(jnp.int32, shape, 0)
        column = lax.broadcasted_iota(jnp.int32, shape, 1)
        half = width // 2
        freq = start + slot // width * half + slot % half
        odd = slot % width >= half
        nyquist = odd & (freq == 0)
        direct = (column == freq - start) & ~nyquist & (column < count)
        mirror = (column - count + high == group_len - freq) & (freq > 0)
        mirror = mirror & (column >= count) & (column < 2 * count + 16)
        middle = nyquist & (column == 2 * count + 16)
        signed = jnp.where(odd, -1.0, 1.0)
        matrix = jnp.where(direct, signed, jnp.where(mirror | middle, 1.0, 0.0)).astype(BF16)
        fold_ref[row_count * offsets[i] : row_count * (offsets[i] + width), :depth] = matrix

    def fold(m):
        if m == 0:
            for i in range(chunks):
                fold_matrix(i)
            w_copy.wait()

        def step(n, carry):
            group = n // pieces
            origin = group * group_len
            cols = rows_of(n % pieces * wide, wide, wide)
            for i in range(chunks):
                start, count, high, depth = fold_spans(i)
                base = row_count * offsets[i]
                taken = [w_ref[rows_of(origin + start, count, 16), cols]]
                taken.append(w_ref[rows_of(origin + high, count + 16, 16), cols])
                if i == 0:
                    taken.append(w_ref[rows_of(origin + group_len // 2, 16, 16), cols])
                value = jnp.dot(
                    fold_ref[base : base + 2 * count, :depth], jnp.concatenate(taken, 0),
                    preferred_element_type=F32,
                ).astype(BF16)
                for s in range(2):
                    start = base * col_count + s * col_count * count + group * count
                    folded[rows_of(start, count, 16), cols] = value[s * count : (s + 1) * count]
            return carry

        lax.fori_loop(FOLDS[m], FOLDS[m + 1], step, 0)

    done = []

    def multiply(i, h):
        width, offset = WIDTHS[i], offsets[i]
        count = quads * width
        depth = col_count * count
        arrived(held.at[:2, :, place_of(i, h), :], g_recv.at[2 * i + (h == "f"), 2])
        for g in range(col_count):
            for q in range(quads):
                lhs[q * 128 : (q + 1) * 128, g * count : (g + 1) * count] = jnp.transpose(
                    held[g, q, place_of(i, h), :]
                )
        where = side if h == "n" else 1 - side
        rows = rows_of(row_count * offset * col_count + where * depth, depth, 16)
        first, last = not done, len(done) == 2 * chunks - 1
        done.append((i, h))

        def step(n, carry):
            cols = rows_of(n * broad, broad, broad)
            value = jnp.dot(lhs[:, :depth], folded[rows, cols], preferred_element_type=F32)
            if not first:
                value = acc[:, cols] + value
            if not last:
                acc[:, cols] = value
            else:
                out_ref[:, :, cols] = value.astype(BF16).reshape(row_count, part, broad)
            return carry

        lax.fori_loop(0, out_width // broad, step, 0)

    for token in PLAN:
        i = int(token[-1]) if token[-1].isdigit() else 0
        with jax.named_scope(token):
            match token[0]:
                case "A":
                    first_exchange(i)
                case "I":
                    inverses()
                case "F":
                    fold(i)
                case "D":
                    transform(i)
                case "G":
                    gather(i, token[1])
                case "X":
                    forward(i, token[1])
                case "M":
                    multiply(i, token[1])

    sent(sums.at[: col_count - 1], 0)
    sent(invs.at[: row_count - 1], 1)
    sent(send1.at[: group_len - slab], 2)
    sent(send2.at[: row_count - 1], 3)
    sent(held.at[: col_count - 1], 4)


def on_device_fused(tokens, norm_gain, out_weight):
    row_count = lax.axis_size("row")
    col_count = lax.axis_size("col")
    block_len, group_len = tokens.shape
    out_width = out_weight.shape[1]
    slab = group_len // row_count
    part = block_len // row_count
    chunks = len(WIDTHS)
    widest = max(WIDTHS)
    chan_table, low_table, twist = fused_tables(group_len, row_count, block_len)
    vmem = pl.BlockSpec(memory_space=pltpu.VMEM)
    hbm = pl.BlockSpec(memory_space=pl.ANY)
    dma = pltpu.SemaphoreType.DMA
    mapped = pl.pallas_call(
        functools.partial(fused_kernel, (row_count, col_count)),
        out_shape=pltpu.VMEM((row_count, part, out_width), BF16),
        in_specs=[hbm] * 6,
        out_specs=vmem,
        scratch_shapes=[
            pltpu.VMEM((block_len, group_len), BF16),
            pltpu.VMEM((1, group_len), F32),
            pltpu.VMEM(twist.shape, F32),
            pltpu.VMEM((block_len, group_len), BF16),
            pltpu.VMEM(chan_table.shape, BF16),
            pltpu.VMEM(low_table.shape, BF16),
            pltpu.VMEM(out_weight.shape, BF16),
            pltpu.VMEM((group_len, row_count * widest + 32), BF16),
            pltpu.VMEM(out_weight.shape, BF16),
            pltpu.VMEM((group_len, block_len), BF16),
            pltpu.VMEM((row_count, slab, block_len), BF16),
            pltpu.VMEM((col_count, 1, block_len), F32),
            pltpu.VMEM((row_count, 1, block_len), F32),
            pltpu.VMEM((row_count * widest, 2 * block_len), BF16),
            pltpu.VMEM((row_count, row_count // 2, slab, 128), BF16),
            pltpu.VMEM((col_count, row_count // 2, group_len, 128), BF16),
            pltpu.VMEM((block_len, col_count * row_count // 2 * widest), BF16),
            pltpu.VMEM((block_len, out_width), F32),
            dma((7,)), dma((2, chunks)), dma((5,)), dma((1,)), dma((1,)),
            dma((chunks,)), dma((chunks, 2)), dma((2 * chunks, 3)),
        ],
        compiler_params=pltpu.CompilerParams(
            collective_id=0, has_side_effects=True, vmem_limit_bytes=60 * 1024 * 1024
        ),
    )(
        tokens, norm_gain[None, :], jnp.asarray(chan_table, BF16), jnp.asarray(low_table, BF16),
        jnp.asarray(twist, F32), out_weight,
    )
    return jnp.transpose(mapped, (1, 0, 2)).reshape(block_len, out_width)


def on_device(tokens, norm_gain, out_weight):
    row_count = lax.axis_size("row")
    col_count = lax.axis_size("col")
    block_len, local_width = tokens.shape
    full_width = local_width * col_count
    group_len = full_width // GROUPS
    share_len = block_len // col_count
    seq_len = block_len * row_count
    slab_len = full_width // row_count
    col_index = lax.axis_index("col")
    chan_idx = jnp.arange(group_len, dtype=jnp.int32)
    cosines, sines = phases(chan_idx, chan_idx, group_len)
    chan_table = jnp.concatenate([cosines, sines], axis=1) / math.sqrt(group_len)
    table_parts = split_table(chan_table)
    arranged = tokens.reshape(col_count, share_len, local_width)
    portion = lax.all_to_all(arranged, "col", split_axis=0, concat_axis=2, tiled=True)
    item_count = portion.shape[1]
    values = portion.astype(jnp.float32)
    inv_rms = lax.rsqrt(jnp.mean(values * values, axis=-1, keepdims=True) + EPSILON)
    normed = lax.optimization_barrier((values * inv_rms * norm_gain).astype(jnp.bfloat16))
    grouped = normed.reshape(item_count, GROUPS, group_len)
    result = jnp.einsum("pgm,mj->pgj", grouped, table_parts[0], preferred_element_type=jnp.float32)
    result = result + jnp.einsum(
        "pgm,mj->pgj", grouped, table_parts[1], preferred_element_type=jnp.float32
    )
    result = result + jnp.einsum(
        "pgm,mj->pgj", grouped, table_parts[2], preferred_element_type=jnp.float32
    )
    high_idx = jnp.arange(row_count, dtype=jnp.int32)
    high_cos, high_sin = phases(high_idx, high_idx, row_count)
    high_table = jnp.concatenate(
        [jnp.concatenate([high_cos, -high_sin], 1), jnp.concatenate([-high_sin, -high_cos], 1)], 0
    )
    parts = (
        lax.all_to_all(
            result[..., :group_len].reshape(1, item_count, full_width),
            "row",
            split_axis=2,
            concat_axis=0,
            tiled=True,
        ),
        lax.all_to_all(
            result[..., group_len:].reshape(1, item_count, full_width),
            "row",
            split_axis=2,
            concat_axis=0,
            tiled=True,
        ),
    )
    item_count = parts[0].shape[1]
    stacked = jnp.concatenate(parts, 0).reshape(2 * row_count, item_count * slab_len)
    result = jnp.dot(high_table, stacked, precision=PRECISE)
    real_part = result[:row_count].reshape(row_count, item_count, slab_len)
    imag_part = result[row_count:].reshape(row_count, item_count, slab_len)
    local_pos = col_index * share_len + jnp.arange(share_len, dtype=jnp.int32)
    twist_cos, twist_sin = phases(high_idx, local_pos, seq_len)
    twist_cos = twist_cos[:, :, None]
    twist_sin = twist_sin[:, :, None]
    turned_real = real_part * twist_cos + imag_part * twist_sin
    turned_imag = imag_part * twist_cos - real_part * twist_sin
    low_idx = jnp.arange(block_len, dtype=jnp.int32)
    low_cos, low_sin = phases(low_idx, low_idx, block_len)
    low_cos = low_cos / math.sqrt(seq_len)
    low_sin = low_sin / math.sqrt(seq_len)
    low_table = jnp.concatenate([low_cos, low_sin], 1)
    stacked = jnp.concatenate(
        (
            lax.all_to_all(turned_real, "col", split_axis=0, concat_axis=1, tiled=True),
            lax.all_to_all(turned_imag, "col", split_axis=0, concat_axis=1, tiled=True),
        ),
        1,
    )
    finished = (jnp.einsum("ks,asc->akc", low_table, stacked, precision=PRECISE),)[0]
    spectrum = finished.astype(jnp.bfloat16)
    returned = lax.all_to_all(spectrum, "row", split_axis=1, concat_axis=2, tiled=True)
    mapped = jnp.einsum(
        "akd,de->kae",
        lax.all_gather(returned, "col", axis=0, tiled=True),
        out_weight,
        preferred_element_type=jnp.float32,
    )
    return mapped.astype(jnp.bfloat16).reshape(block_len, local_width)


def solution(mesh):
    def body(tokens, norm_gain, out_weight):
        whole_groups = tokens.shape[1] * GROUPS == out_weight.shape[0]
        slab = tokens.shape[1] // mesh.shape["row"]
        program = on_device_folded if whole_groups else on_device
        if whole_groups and slab == 128 and mesh.shape["col"] == 4 and mesh.shape["row"] == 8:
            program = on_device_fused
        return program(tokens, norm_gain, out_weight)

    placed = (P("row", "col"), P(), P(None, "col"))
    return jax.shard_map(
        body, mesh=mesh, in_specs=placed, out_specs=P("row", "col"), check_vma=False
    )
```
